32 devices in a mesh: sp: 4 (over y, x), tp: 8 (over z, core).
Axes of the slice: x: 2, y: 2, z: 4, core: 2. Of those that a mesh axis runs over, the one named last changes fastest.
Arguments:
- latent: bfloat16 [4096, 2048], P(('sp', 'tp')), may hold values from -1.5 to 1.5
- context: bfloat16 [128, 2048], P('sp'), may hold values from -6 to 6
- cond: bfloat16 [2048], replicated, may hold values from -6 to 6
- cond_context: bfloat16 [2048], replicated, may hold values from -6 to 6
- mod_weight: bfloat16 [3, 2048, 2048], P(None, 'sp', 'tp'), may hold values from -0.125 to 0.125
- norm_gain: bfloat16 [2048], replicated, may hold values from 0.099609375 to 1.8984375
- down_q: bfloat16 [2048, 768], P('tp'), may hold values from -0.125 to 0.125
- down_kv: bfloat16 [2048, 512], P('tp'), may hold values from -0.125 to 0.125
- rope_weight: bfloat16 [2048, 32], replicated, may hold values from -0.125 to 0.125
- qlat_gain: bfloat16 [768], replicated, may hold values from 0.099609375 to 1.8984375
- kvlat_gain: bfloat16 [512], replicated, may hold values from 0.099609375 to 1.8984375
- up_query: bfloat16 [768, 1536], P(None, 'tp'), may hold values from -0.21875 to 0.21875
- up_key: bfloat16 [512, 1024], P(None, 'tp'), may hold values from -0.25 to 0.25
- up_value: bfloat16 [512, 1024], P(None, 'tp'), may hold values from -0.25 to 0.25
- query_gain: float32 [96], replicated, may hold values from 0.5 to 8
- key_gain: float32 [96], replicated, may hold values from 0.5 to 8
- context_bias: float32 [16], P('tp'), may hold values from -2.2 to -0.7
- out_weight: bfloat16 [1024, 2048], P('tp'), may hold values from -24 to 24
Outputs:
- mixed: bfloat16 [4096, 2048], P(('sp', 'tp'))
The draws below stay inside these ranges and needn't reach their ends.
All inputs are finite; a program needn't handle non-finite values.
Results may differ from the reference program's by a relative error of at most 0.028.
The reference program's roundings to bfloat16 on the way count: a program that leaves them out, or rounds other values in their place, can miss the bound.
Values may be sent and summed in bfloat16 or wider, within the bound.
A program may use at most 64 MiB of HBM per device.

```python
import math
import jax
import jax.numpy as jnp
from jax import lax

D = 2048
HEADS = 16
NOPE = 64
ROPE = 32
VDIM = 64
QRANK = 768
KVRANK = 512
GRID_W = 64
TOK_DEV = 1024
CTX_DEV = 32
TOKENS = 4096
CONTEXT = 128


def draw_gain_vector(key):
    return jax.random.uniform(key, (NOPE + ROPE,), jnp.float32, 1.1, 1.9)


def draw_query_gain(key, part):
    return draw_gain_vector(jax.random.fold_in(key, 11))


def draw_key_gain(key, part):
    return draw_gain_vector(jax.random.fold_in(key, 23))


def level_of(own_key, shape, cuts, smallest, largest):
    level = 1.0
    for position, blocks in cuts:
        heights = jax.random.uniform(jax.random.fold_in(jax.random.fold_in(own_key, 6), position), (blocks,), jnp.float32, smallest / len(cuts), largest / len(cuts))
        level = level * jnp.repeat(jnp.exp(heights), shape[position] // blocks).reshape((-1,) + (1,) * (len(shape) - 1 - position))
    return level


def bell_draw(own_key, shape, deviation, bound, cuts=(), held_as=jnp.bfloat16):
    level = level_of(own_key, shape, cuts, -0.22, 0.18) if cuts else 1.0
    result = jax.random.normal(own_key, shape, jnp.float32) * deviation * level
    return jnp.minimum(jnp.maximum(result, -bound), bound).astype(held_as)


def setup_inputs(seed: int = 0) -> dict:
    streams_of = jax.random.split(jax.random.key(seed), 19)
    latent = bell_draw(streams_of[0], (TOKENS, D), 0.25, 1.5, ((0, 32),))
    context = bell_draw(streams_of[1], (CONTEXT, D), 1.0, 6.0, ((0, 4),))
    cond = bell_draw(streams_of[2], (D,), 1.0, 6.0)
    cond_context = bell_draw(streams_of[3], (D,), 1.0, 6.0)
    mod_weight = bell_draw(streams_of[4], (3, D, D), D ** -0.5, 0.125, ((1, 4), (2, 8)))
    norm_gain = jnp.clip(1.0 + 0.18 * jax.random.normal(streams_of[5], (D,), jnp.float32), 0.099609375, 1.8984375).astype(jnp.bfloat16)
    down_q = bell_draw(streams_of[6], (D, QRANK), D ** -0.5, 0.125, ((0, 8),))
    down_kv = bell_draw(streams_of[7], (D, KVRANK), D ** -0.5, 0.125, ((0, 8),))
    rope_weight = bell_draw(streams_of[8], (D, ROPE), D ** -0.5, 0.125)
    qlat_gain = jnp.clip(1.0 + 0.18 * jax.random.normal(streams_of[9], (QRANK,), jnp.float32), 0.099609375, 1.8984375).astype(jnp.bfloat16)
    kvlat_gain = jnp.clip(1.0 + 0.18 * jax.random.normal(streams_of[10], (KVRANK,), jnp.float32), 0.099609375, 1.8984375).astype(jnp.bfloat16)
    up_query = bell_draw(streams_of[11], (QRANK, HEADS * (NOPE + ROPE)), QRANK ** -0.5, 0.21875, ((1, 8),))
    up_key = bell_draw(streams_of[12], (KVRANK, HEADS * NOPE), KVRANK ** -0.5, 0.25, ((1, 8),))
    up_value = bell_draw(streams_of[13], (KVRANK, HEADS * VDIM), KVRANK ** -0.5, 0.25, ((1, 8),))
    query_gain = draw_query_gain(jax.random.fold_in(streams_of[18], 71), 0)
    key_gain = draw_key_gain(jax.random.fold_in(streams_of[18], 71), 0)
    context_bias = jnp.clip(-2.2 + 1.5 * jax.random.uniform(streams_of[16], (HEADS,), jnp.float32) ** level_of(streams_of[16], (HEADS,), ((0, 8),), -0.2, 0.2), -2.2, -0.7)
    out_weight = bell_draw(streams_of[17], (HEADS * VDIM, D), (2.0 * (TOKENS + CONTEXT) ** 0.5 * (HEADS * VDIM) ** -0.5), 24.0, ((0, 8),))
    return dict(latent=latent, context=context, cond=cond, cond_context=cond_context, mod_weight=mod_weight, norm_gain=norm_gain, down_q=down_q, down_kv=down_kv, rope_weight=rope_weight, qlat_gain=qlat_gain, kvlat_gain=kvlat_gain, up_query=up_query, up_key=up_key, up_value=up_value, query_gain=query_gain, key_gain=key_gain, context_bias=context_bias, out_weight=out_weight)


epsilon = 1e-06
theta = 10000.0

def rounded(tensor):
    return lax.optimization_barrier(tensor.astype(jnp.bfloat16))

def rms_scale(tensor, gain):
    return tensor * lax.rsqrt(lax.optimization_barrier(jnp.mean(tensor * tensor, axis=-1, keepdims=True)) + epsilon) * gain.astype(jnp.float32)

def axial_tables(positions):
    pair_count = ROPE // 4
    frequency = jnp.power(theta, -jnp.arange(pair_count, dtype=jnp.float32) / pair_count)
    row_angle = (positions // GRID_W).astype(jnp.float32)[:, None] * frequency
    col_angle = (positions % GRID_W).astype(jnp.float32)[:, None] * frequency
    return (jnp.cos(row_angle), jnp.sin(row_angle), jnp.cos(col_angle), jnp.sin(col_angle))

def rotate_half(tensor, cosine, sine_table):
    first, second = jnp.split(tensor, 2, axis=-1)
    cosine = cosine[:, None, :]
    sine_table = sine_table[:, None, :]
    return jnp.concatenate([first * cosine - second * sine_table, second * cosine + first * sine_table], axis=-1)

def axial_rotate(tensor, tables):
    half_width = tensor.shape[-1] // 2
    return jnp.concatenate([rotate_half(tensor[..., :half_width], tables[0], tables[1]), rotate_half(tensor[..., half_width:], tables[2], tables[3])], axis=-1)

def modulate(row_block, gain, shifts, scales):
    normal = rms_scale(row_block.astype(jnp.float32), gain)
    return rounded(normal * (1.0 + scales) + shifts)

def make_queries(query_latent, up_query, query_gain, tables):
    amount = query_latent.shape[0]
    projected = jnp.dot(query_latent, up_query, preferred_element_type=jnp.float32).reshape(amount, -1, NOPE + ROPE)
    normal = rms_scale(projected, query_gain)
    return rounded(jnp.concatenate([normal[..., :NOPE], axial_rotate(normal[..., NOPE:], tables)], axis=-1))

def make_keys(kv_latent, rope_rows, up_key, up_value, key_gain, tables):
    amount = kv_latent.shape[0]
    unrotated = jnp.dot(kv_latent, up_key, preferred_element_type=jnp.float32).reshape(amount, -1, NOPE)
    head_count = unrotated.shape[1]
    shared = jnp.broadcast_to(rope_rows.astype(jnp.float32)[:, None, :], (amount, head_count, ROPE))
    normal = rms_scale(jnp.concatenate([unrotated, shared], axis=-1), key_gain)
    if tables is not None:
        normal = jnp.concatenate([normal[..., :NOPE], axial_rotate(normal[..., NOPE:], tables)], axis=-1)
    values = jnp.dot(kv_latent, up_value, preferred_element_type=jnp.float32).reshape(amount, head_count, VDIM)
    return (rounded(normal), rounded(values))

def attend(query_block, keys, values, context_keys, context_values, context_shift):
    scaling = (NOPE + ROPE) ** (-0.5)
    query_wide = query_block.astype(jnp.float32)
    latent_scores = jnp.einsum('qhd,khd->qhk', query_wide, keys.astype(jnp.float32)) * scaling
    context_scores = jnp.einsum('qhd,khd->qhk', query_wide, context_keys.astype(jnp.float32)) * scaling
    context_scores = context_scores + context_shift[None, :, None]
    row_max = jnp.maximum(lax.optimization_barrier(jnp.max(latent_scores, axis=-1)), lax.optimization_barrier(jnp.max(context_scores, axis=-1)))[..., None]
    latent_weights = jnp.exp(latent_scores - row_max)
    context_weights = jnp.exp(context_scores - row_max)
    totals = lax.optimization_barrier(jnp.sum(latent_weights, axis=-1)) + lax.optimization_barrier(jnp.sum(context_weights, axis=-1))
    summed = jnp.einsum('qhk,khd->qhd', rounded(latent_weights).astype(jnp.float32), values.astype(jnp.float32))
    summed = summed + jnp.einsum('qhk,khd->qhd', rounded(context_weights).astype(jnp.float32), context_values.astype(jnp.float32))
    return rounded(summed / totals[..., None])

def reference(latent, context, cond, cond_context, mod_weight, norm_gain, down_q, down_kv, rope_weight, qlat_gain, kvlat_gain, up_query, up_key, up_value, query_gain, key_gain, context_bias, out_weight):
    activated = rounded(jax.nn.silu(jnp.stack([cond, cond_context]).astype(jnp.float32)))
    shifts, scales, gates = (jnp.dot(activated[0], mod_weight[member], preferred_element_type=jnp.float32) for member in range(3))
    context_shift, context_scale = (jnp.dot(activated[1], mod_weight[member], preferred_element_type=jnp.float32) for member in range(2))
    normed = modulate(latent, norm_gain, shifts, scales)
    context_normed = modulate(context, norm_gain, context_shift, context_scale)
    query_latent = rounded(rms_scale(jnp.dot(normed, down_q, preferred_element_type=jnp.float32), qlat_gain))
    kv_latent = rounded(rms_scale(jnp.dot(normed, down_kv, preferred_element_type=jnp.float32), kvlat_gain))
    context_kv = rounded(rms_scale(jnp.dot(context_normed, down_kv, preferred_element_type=jnp.float32), kvlat_gain))
    rope_rows = rounded(jnp.dot(normed, rope_weight, preferred_element_type=jnp.float32))
    context_rope = rounded(jnp.dot(context_normed, rope_weight, preferred_element_type=jnp.float32))
    tables = axial_tables(jnp.arange(TOKENS, dtype=jnp.int32))
    queries = make_queries(query_latent, up_query, query_gain, tables)
    keys, values = make_keys(kv_latent, rope_rows, up_key, up_value, key_gain, tables)
    context_keys, context_values = make_keys(context_kv, context_rope, up_key, up_value, key_gain, None)
    context_shift_heads = context_bias.astype(jnp.float32) + math.log(TOK_DEV / CTX_DEV)
    block_rows = math.gcd(TOKENS, 256)
    query_blocks = queries.reshape(TOKENS // block_rows, block_rows, HEADS, NOPE + ROPE)
    attended = lax.map(lambda blocks: attend(blocks, keys, values, context_keys, context_values, context_shift_heads), query_blocks)
    attended = attended.reshape(TOKENS, HEADS * VDIM)
    projected = jnp.dot(attended, out_weight, preferred_element_type=jnp.float32)
    return (latent.astype(jnp.float32) + gates * projected).astype(jnp.bfloat16)
```

```python
import math

import jax
import jax.numpy as jnp
from jax import lax
from jax.experimental import pallas as pl
from jax.experimental.pallas import tpu as pltpu
from jax.sharding import PartitionSpec as P

NOPE = 64
ROPE = 32
VDIM = 64
GRID_W = 64
TOK_DEV = 1024
CTX_DEV = 32


epsilon = 1e-06
theta = 10000.0


def rms_scale(tensor, gain):
    return (
        tensor
        * lax.rsqrt(jnp.mean(tensor * tensor, axis=-1, keepdims=True) + epsilon)
        * gain.astype(jnp.float32)
    )


def axial_tables(positions):
    pair_count = ROPE // 4
    frequency = jnp.power(theta, -jnp.arange(pair_count, dtype=jnp.float32) / pair_count)
    row_angle = (positions // GRID_W).astype(jnp.float32)[:, None] * frequency
    col_angle = (positions % GRID_W).astype(jnp.float32)[:, None] * frequency
    return (jnp.cos(row_angle), jnp.sin(row_angle), jnp.cos(col_angle), jnp.sin(col_angle))


def rotate_half(tensor, cosine, sine_table):
    first, second = jnp.split(tensor, 2, axis=-1)
    cosine = cosine[:, None, :]
    sine_table = sine_table[:, None, :]
    return jnp.concatenate(
        [first * cosine - second * sine_table, second * cosine + first * sine_table], axis=-1
    )


def axial_rotate(tensor, tables):
    half_width = tensor.shape[-1] // 2
    return jnp.concatenate(
        [
            rotate_half(tensor[..., :half_width], tables[0], tables[1]),
            rotate_half(tensor[..., half_width:], tables[2], tables[3]),
        ],
        axis=-1,
    )


def modulate(row_block, gain, shifts, scales):
    normal = rms_scale(row_block.astype(jnp.float32), gain)
    return (normal * (1.0 + scales) + shifts).astype(jnp.bfloat16)


def make_queries(query_latent, up_query, query_gain, tables):
    amount = query_latent.shape[0]
    projected = jnp.dot(query_latent, up_query, preferred_element_type=jnp.float32).reshape(
        amount, -1, NOPE + ROPE
    )
    normal = rms_scale(projected, query_gain)
    return jnp.concatenate(
        [normal[..., :NOPE], axial_rotate(normal[..., NOPE:], tables)], axis=-1
    ).astype(jnp.bfloat16)


def make_keys(kv_latent, rope_rows, up_key, up_value, key_gain, tables):
    amount = kv_latent.shape[0]
    unrotated = jnp.dot(kv_latent, up_key, preferred_element_type=jnp.float32).reshape(
        amount, -1, NOPE
    )
    head_count = unrotated.shape[1]
    shared = jnp.broadcast_to(rope_rows.astype(jnp.float32)[:, None, :], (amount, head_count, ROPE))
    normal = rms_scale(jnp.concatenate([unrotated, shared], axis=-1), key_gain)
    if tables is not None:
        normal = jnp.concatenate(
            [normal[..., :NOPE], axial_rotate(normal[..., NOPE:], tables)], axis=-1
        )
    values = jnp.dot(kv_latent, up_value, preferred_element_type=jnp.float32).reshape(
        amount, head_count, VDIM
    )
    return (normal.astype(jnp.bfloat16), values.astype(jnp.bfloat16))


CORES = 2


def greet(sp_peers=True):
    sp, tp = lax.axis_index("sp"), lax.axis_index("tp")
    S, T = lax.axis_size("sp"), lax.axis_size("tp")
    barrier = pltpu.get_barrier_semaphore()
    for k in range(1, S):
        pl.semaphore_signal(barrier, inc=1, device_id={"sp": lax.rem(sp + k, S)}, device_id_type=pl.DeviceIdType.MESH)
    for k in range(1, T):
        pl.semaphore_signal(barrier, inc=1, device_id={"tp": lax.rem(tp + k, T)}, device_id_type=pl.DeviceIdType.MESH)
    pl.semaphore_wait(barrier, S + T - 2)


def remote(source, target, send, recv, device):
    return pltpu.make_async_remote_copy(
        src_ref=source,
        dst_ref=target,
        send_sem=send,
        recv_sem=recv,
        device_id=device,
        device_id_type=pl.DeviceIdType.MESH,
    )


class Line:
    def __init__(self, own, slots, send, recv, z, core, Z):
        self.own, self.slots, self.send, self.recv = own, slots, send, recv
        self.z, self.core, self.Z = z, core, Z

    def hop(self, block, step, first=False):
        to = lax.max(lax.min(self.z + step, self.Z - 1), 0)
        d = 0 if step > 0 else 1
        return remote(
            self.own if first else self.slots(block),
            self.slots(block),
            self.send.at[block, d],
            self.recv.at[block],
            {"tp": to * CORES + self.core},
        )

    def start(self):
        for step in (1, -1):
            ok = (self.z + step >= 0) & (self.z + step < self.Z)

            @pl.when(ok)
            def _():
                self.hop(self.z, step, True).start()

    def each(self, body):
        for k in range(1, self.Z):
            for step in (1, -1):
                block = self.z - step * k

                @pl.when((block >= 0) & (block < self.Z))
                def _():
                    body(block, step)

    def arrive(self, block, step):
        self.hop(block, step).wait_recv()
        ok = (self.z + step >= 0) & (self.z + step < self.Z)

        @pl.when(ok)
        def _():
            self.hop(block, step).start()

    def drain(self):
        for step in (1, -1):
            ok = (self.z + step >= 0) & (self.z + step < self.Z)

            @pl.when(ok)
            def _():
                self.hop(self.z, step, True).wait_send()

        def body(block, step):
            ok = (self.z + step >= 0) & (self.z + step < self.Z)

            @pl.when(ok)
            def _():
                self.hop(block, step).wait_send()

        self.each(body)


def loop(low, high, body):
    def step(k, carry):
        body(k)
        return carry

    lax.fori_loop(low, high, step, 0)


def weights_kernel(
    part, dq, dkv, ow, mods, dq_all, dkv_all, ow_part,
    pm, msum, m_send, m_recv, t_send, t_recv, l_send, l_recv, s_send, s_recv, c_send, c_recv, loc,
):
    sp, tp = lax.axis_index("sp"), lax.axis_index("tp")
    S, T = lax.axis_size("sp"), lax.axis_size("tp")
    Z = T // CORES
    z, core = tp // CORES, lax.rem(tp, CORES)
    mate = {"tp": tp + 1 - 2 * core}
    greet()
    downs = ((dq, dq_all), (dkv, dkv_all))

    def part_copy(k):
        return remote(part, pm.at[sp], m_send.at[k], m_recv.at[k], {"sp": lax.rem(sp + k, S)})

    loop(1, S, lambda k: part_copy(k).start())
    lines = [
        Line(a.at[sp], (lambda o: lambda b: o.at[b, core, sp])(o), l_send.at[i], l_recv.at[i], z, core, Z)
        for i, (a, o) in enumerate(downs)
    ]
    lines.append(Line(ow.at[sp], lambda b: ow_part.at[b], l_send.at[2], l_recv.at[2], z, core, Z))
    for line in lines[:2]:
        line.start()
    local = []
    for i, (a, o) in enumerate(downs):
        local.append(pltpu.make_async_copy(a, o.at[z, core], loc.at[i]))
    local.append(pltpu.make_async_copy(ow.at[sp], ow_part.at[z], loc.at[2]))
    for copy in local:
        copy.start()

    def mate_copy(i, block, own=False):
        a, o = downs[i]
        return remote(
            a if own else o.at[block, core], o.at[block, core], c_send.at[i, block], c_recv.at[i, block], mate
        )

    def mate_wait(i, block):
        a, o = downs[i]
        to = o.at[block, 1 - core]
        remote(to, to, c_send.at[i, block], c_recv.at[i, block], mate).wait_recv()

    for i in range(2):
        mate_copy(i, z, True).start()
    pm[sp] = part[...]
    loop(1, S, lambda k: part_copy(k).wait_recv())
    total = pm[0]
    for k in range(1, S):
        total = total + pm[k]
    msum[...] = total
    mods[tp] = total

    def spread(i, block, k):
        at = downs[i][1].at[block, core, sp]
        return remote(at, at, s_send.at[i, block, k], s_recv.at[i, block, k], {"sp": lax.rem(sp + k, S)})

    def gathered(i, block, k):
        at = downs[i][1].at[block, core, lax.rem(sp - k + S, S)]
        return remote(at, at, s_send.at[i, block, k], s_recv.at[i, block, k], {"sp": lax.rem(sp + k, S)})

    def body(block, step):
        for i in range(2):
            lines[i].arrive(block, step)
            loop(1, S, lambda k: spread(i, block, k).start())

    def mod_copy(k):
        return remote(msum, mods.at[tp], t_send.at[k], t_recv.at[k], {"tp": lax.rem(tp + k, T)})

    def mod_wait(k):
        to = mods.at[lax.rem(tp - k + T, T)]
        remote(msum, to, t_send.at[k], t_recv.at[k], {"tp": lax.rem(tp + k, T)}).wait_recv()

    loop(1, T, lambda k: mod_copy(k).start())
    lines[0].each(body)
    lines[2].start()
    lines[2].each(lines[2].arrive)

    def body(block, step):
        for i in range(2):
            loop(1, S, lambda k: gathered(i, block, k).wait_recv())
            mate_copy(i, block).start()

    lines[0].each(body)
    for copy in local:
        copy.wait()
    loop(1, T, mod_wait)
    for i in range(2):
        for b in range(Z):
            mate_wait(i, b)
    for i in range(2):
        mate_copy(i, z, True).wait_send()

    def body(block, step):
        for i in range(2):
            mate_copy(i, block).wait_send()
            loop(1, S, lambda k: spread(i, block, k).wait_send())

    lines[0].each(body)
    for line in lines:
        line.drain()
    loop(1, S, lambda k: part_copy(k).wait_send())
    loop(1, T, lambda k: mod_copy(k).wait_send())


def latents_kernel(lat, ow_part, lat_all, ow_all, l_send, l_recv, s_send, s_recv, c_send, c_recv, loc):
    sp, tp = lax.axis_index("sp"), lax.axis_index("tp")
    S, T = lax.axis_size("sp"), lax.axis_size("tp")
    Z = T // CORES
    z, core = tp // CORES, lax.rem(tp, CORES)
    mate = {"tp": tp + 1 - 2 * core}
    greet()
    line = Line(lat, lambda b: lat_all.at[b, core], l_send, l_recv, z, core, Z)
    line.start()

    def mate_copy(block, own=False):
        to = lat_all.at[block, core]
        return remote(lat if own else to, to, c_send.at[block], c_recv.at[block], mate)

    mate_copy(z, True).start()

    def spread(k):
        return remote(ow_part, ow_all.at[:, core, sp], s_send.at[k], s_recv.at[k], {"sp": lax.rem(sp + k, S)})

    def gathered(k):
        to = ow_all.at[:, core, lax.rem(sp - k + S, S)]
        return remote(ow_part, to, s_send.at[k], s_recv.at[k], {"sp": lax.rem(sp + k, S)})

    loop(1, S, lambda k: spread(k).start())
    own_lat = pltpu.make_async_copy(lat, lat_all.at[z, core], loc.at[0])
    own_ow = pltpu.make_async_copy(ow_part, ow_all.at[:, core, sp], loc.at[1])
    own_lat.start()
    own_ow.start()

    def body(block, step):
        line.arrive(block, step)
        mate_copy(block).start()

    line.each(body)
    own_lat.wait()
    own_ow.wait()
    loop(1, S, lambda k: gathered(k).wait_recv())
    whole = remote(ow_all.at[:, core], ow_all.at[:, core], c_send.at[Z], c_recv.at[Z], mate)
    whole.start()
    for b in range(Z):
        to = lat_all.at[b, 1 - core]
        remote(to, to, c_send.at[b], c_recv.at[b], mate).wait_recv()
    to = ow_all.at[:, 1 - core]
    remote(to, to, c_send.at[Z], c_recv.at[Z], mate).wait_recv()
    whole.wait_send()
    mate_copy(z, True).wait_send()
    line.each(lambda block, step: mate_copy(block).wait_send())
    line.drain()
    loop(1, S, lambda k: spread(k).wait_send())


def attend_kernel(
    q, kv, ctx, shift, out, kv_all, ctx_all, m_scr, l_scr, acc, att,
    k_send, k_recv, x_send, x_recv, a_send, a_recv,
):
    sp, tp = lax.axis_index("sp"), lax.axis_index("tp")
    S, T = lax.axis_size("sp"), lax.axis_size("tp")
    H, N, KD = q.shape
    rows = out.shape[1]
    TQ = math.gcd(N, 256)
    WIDE = KD + VDIM
    factor = KD ** (-0.5) * math.log2(math.e)
    greet()

    def ctx_copy(k):
        return remote(ctx, ctx_all.at[sp], x_send.at[k], x_recv.at[k], {"sp": lax.rem(sp + k, S)})

    def ctx_wait(k):
        to = ctx_all.at[lax.rem(sp - k + S, S)]
        remote(ctx, to, x_send.at[k], x_recv.at[k], {"sp": lax.rem(sp + k, S)}).wait_recv()

    def kv_copy(k):
        return remote(kv, kv_all.at[sp], k_send.at[k], k_recv.at[k], {"sp": lax.rem(sp + k, S)})

    loop(1, S, lambda k: ctx_copy(k).start())
    loop(1, S, lambda k: kv_copy(k).start())

    def lanes(p):
        total = p[:, :128]
        for j in range(1, p.shape[1] // 128):
            total = total + p[:, j * 128 : (j + 1) * 128]
        return total

    def first(qi):
        at = pl.ds(pl.multiple_of(qi * TQ, TQ), TQ)
        for h in range(H):
            kt = kv[h * WIDE : h * WIDE + KD, :]
            vt = kv[h * WIDE + KD : (h + 1) * WIDE, :]
            s = jnp.dot(q[h, at, :], kt, preferred_element_type=jnp.float32) * factor
            new = jnp.max(s, axis=1, keepdims=True)
            p = jnp.exp2(s - new)
            m_scr[h, at, :] = jnp.broadcast_to(new, (TQ, 128))
            l_scr[h, at, :] = lanes(p)
            acc[h, at, :] = lax.dot_general(
                p.astype(jnp.bfloat16), vt, (((1,), (1,)), ((), ())), preferred_element_type=jnp.float32
            )

    loop(0, N // TQ, first)

    def absorb(h, at, s, value, dims):
        old = m_scr[h, at, :][:, :1]
        new = jnp.maximum(old, jnp.max(s, axis=1, keepdims=True))
        scale = jnp.exp2(old - new)
        p = jnp.exp2(s - new)
        m_scr[h, at, :] = jnp.broadcast_to(new, (TQ, 128))
        l_scr[h, at, :] = l_scr[h, at, :] * scale + lanes(p)
        acc[h, at, :] = acc[h, at, :] * scale + lax.dot_general(
            p.astype(jnp.bfloat16), value, (dims, ((), ())), preferred_element_type=jnp.float32
        )

    ctx_all[sp] = ctx[...]
    loop(1, S, ctx_wait)

    def context_step(qi):
        at = pl.ds(pl.multiple_of(qi * TQ, TQ), TQ)
        for h in range(H):
            rows_all = ctx_all[...].reshape(-1, ctx_all.shape[2])
            kc = rows_all[:, h * 256 : h * 256 + 128][:, :KD]
            vc = rows_all[:, h * 256 + 128 : h * 256 + 256][:, :VDIM]
            s = lax.dot_general(q[h, at, :], kc, (((1,), (1,)), ((), ())), preferred_element_type=jnp.float32)
            s = s * factor + shift[h : h + 1, :1]
            absorb(h, at, s, vc, ((1,), (0,)))

    loop(0, N // TQ, context_step)

    def latent_step(k):
        slot = lax.rem(sp - k + S, S)
        to = kv_all.at[slot]
        remote(kv, to, k_send.at[k], k_recv.at[k], {"sp": lax.rem(sp + k, S)}).wait_recv()

        def tile(qi):
            at = pl.ds(pl.multiple_of(qi * TQ, TQ), TQ)
            for h in range(H):
                kt = kv_all[slot, h * WIDE : h * WIDE + KD, :]
                vt = kv_all[slot, h * WIDE + KD : (h + 1) * WIDE, :]
                s = jnp.dot(q[h, at, :], kt, preferred_element_type=jnp.float32) * factor
                absorb(h, at, s, vt, ((1,), (1,)))

        loop(0, N // TQ, tile)

    loop(1, S, latent_step)

    def finish(qi):
        at = pl.ds(pl.multiple_of(qi * TQ, TQ), TQ)
        heads = [acc[h, at, :] / jnp.sum(l_scr[h, at, :], axis=1, keepdims=True) for h in range(H)]
        att[at, :] = jnp.concatenate(heads, axis=1).astype(jnp.bfloat16)

    loop(0, N // TQ, finish)

    def give(k):
        peer = lax.rem(tp + k, T)
        return remote(
            att.at[pl.ds(pl.multiple_of(peer * rows, rows), rows)], out.at[tp], a_send.at[k], a_recv.at[k], {"tp": peer}
        )

    def take(k):
        to = out.at[lax.rem(tp - k + T, T)]
        remote(to, to, a_send.at[k], a_recv.at[k], {"tp": lax.rem(tp + k, T)}).wait_recv()

    loop(1, T, lambda k: give(k).start())
    out[tp] = att[pl.ds(pl.multiple_of(tp * rows, rows), rows), :]
    loop(1, T, take)
    loop(1, T, lambda k: give(k).wait_send())
    loop(1, S, lambda k: kv_copy(k).wait_send())
    loop(1, S, lambda k: ctx_copy(k).wait_send())


DMA = pltpu.SemaphoreType.DMA
VM = pl.BlockSpec(memory_space=pltpu.VMEM)
ANY = pl.BlockSpec(memory_space=pl.ANY)


def call(kernel, ident, outs, out_specs, scratch, args):
    return pl.pallas_call(
        kernel,
        out_shape=outs,
        in_specs=[VM] * len(args),
        out_specs=out_specs,
        scratch_shapes=scratch,
        compiler_params=pltpu.CompilerParams(
            collective_id=ident, has_side_effects=True, vmem_limit_bytes=48 * 1024 * 1024
        ),
    )(*args)


def rotated_columns(normal, tables):
    base = NOPE
    m = ROPE // 4
    a, b, c, d = (normal[..., base + i * m : base + (i + 1) * m, :] for i in range(4))
    rc, rs, cc, cs = (table.T for table in tables)
    return jnp.concatenate(
        [normal[..., :base, :], a * rc - b * rs, b * rc + a * rs, c * cc - d * cs, d * cc + c * cs], axis=-2
    )


def norm_columns(u, gain):
    return u * lax.rsqrt(jnp.mean(u * u, axis=-2, keepdims=True) + epsilon) * gain[:, None]


def shards(
    latent, context, cond, cond_context, mod_weight, norm_gain, down_q, down_kv, rope_weight, qlat_gain, kvlat_gain,
    up_query, up_key, up_value, query_gain, key_gain, context_bias, out_weight,
):
    seq_index = lax.axis_index("sp")
    S, T = lax.axis_size("sp"), lax.axis_size("tp")
    Z = T // CORES
    bf16, f32 = jnp.bfloat16, jnp.float32
    own_rows = latent.shape[0]
    block_tokens = own_rows * T
    row_span, cols = mod_weight.shape[1:]
    width = latent.shape[1]
    activated = jax.nn.silu(jnp.stack([cond, cond_context]).astype(f32)).astype(bf16)
    own_part = lax.dynamic_slice_in_dim(activated, seq_index * row_span, row_span, 1)
    both = jnp.einsum("cd,rde->rce", own_part, mod_weight, preferred_element_type=f32)
    partial_value = jnp.concatenate([both.reshape(6, cols), jnp.zeros((2, cols), f32)], axis=0)
    pieces = [w.reshape(S, w.shape[0] // S, w.shape[1]) for w in (down_q, down_kv, out_weight)]
    dq, dkv, ow = pieces
    mods, dq_all, dkv_all, ow_part = call(
        weights_kernel,
        1,
        (
            jax.ShapeDtypeStruct((T, 8, cols), f32),
            jax.ShapeDtypeStruct((Z, CORES) + dq.shape, bf16),
            jax.ShapeDtypeStruct((Z, CORES) + dkv.shape, bf16),
            jax.ShapeDtypeStruct((Z,) + ow.shape[1:], bf16),
        ),
        (VM, ANY, ANY, ANY),
        [
            pltpu.VMEM((S, 8, cols), f32), pltpu.VMEM((8, cols), f32),
            DMA((S,)), DMA((S,)), DMA((T,)), DMA((T,)),
            DMA((3, Z, 2)), DMA((3, Z)), DMA((2, Z, S)), DMA((2, Z, S)), DMA((2, Z)), DMA((2, Z)), DMA((3,)),
        ],
        (partial_value, dq, dkv, ow),
    )
    mods = mods.transpose(1, 0, 2).reshape(8, width)
    normed = modulate(latent, norm_gain, mods[0], mods[2])
    context_normed = modulate(context, norm_gain, mods[1], mods[3])
    gates = mods[4]
    stacked = jnp.concatenate([normed, context_normed], axis=0)
    query_down = jnp.dot(normed, dq_all.reshape(width, -1), preferred_element_type=f32)
    kv_down = jnp.dot(stacked, dkv_all.reshape(width, -1), preferred_element_type=f32)
    query_latent = rms_scale(query_down, qlat_gain).astype(bf16)
    kv_latent = rms_scale(kv_down, kvlat_gain).astype(bf16)
    rope_rows = jnp.dot(stacked, rope_weight, preferred_element_type=f32).astype(bf16)
    QR, KR = query_latent.shape[1], kv_latent.shape[1]
    lat = jnp.concatenate(
        [query_latent, kv_latent[:own_rows], jnp.pad(rope_rows[:own_rows], ((0, 0), (0, 128 - ROPE)))], axis=1
    )
    lat_all, ow_all = call(
        latents_kernel,
        2,
        (
            jax.ShapeDtypeStruct((Z, CORES) + lat.shape, bf16),
            jax.ShapeDtypeStruct((Z, CORES) + ow.shape, bf16),
        ),
        (ANY, ANY),
        [DMA((Z, 2)), DMA((Z,)), DMA((S,)), DMA((S,)), DMA((Z + 1,)), DMA((Z + 1,)), DMA((2,))],
        (lat, ow_part),
    )
    lat_all = lat_all.reshape(block_tokens, -1)
    ctx_keys, ctx_values = make_keys(
        kv_latent[own_rows:], rope_rows[own_rows:], up_key, up_value, key_gain, None
    )
    H = ctx_keys.shape[1]
    KD = NOPE + ROPE
    ctx = jnp.concatenate(
        [jnp.pad(ctx_keys, ((0, 0), (0, 0), (0, 128 - KD))), jnp.pad(ctx_values, ((0, 0), (0, 0), (0, 128 - VDIM)))],
        axis=-1,
    ).reshape(-1, H * 256)
    positions = seq_index * block_tokens + jnp.arange(block_tokens, dtype=jnp.int32)
    tables = axial_tables(positions)
    all_query, all_kv, all_rope = (
        lat_all[:, :QR], lat_all[:, QR : QR + KR], lat_all[:, QR + KR : QR + KR + ROPE]
    )
    uq = lax.dot_general(up_query, all_query, (((0,), (1,)), ((), ())), preferred_element_type=f32)
    queries = rotated_columns(norm_columns(uq.reshape(H, KD, -1), query_gain), tables).astype(bf16)
    queries = queries.transpose(0, 2, 1)
    uk = lax.dot_general(up_key, all_kv, (((0,), (1,)), ((), ())), preferred_element_type=f32)
    shared = jnp.broadcast_to(all_rope.astype(f32).T[None], (H, ROPE, block_tokens))
    keys = norm_columns(jnp.concatenate([uk.reshape(H, NOPE, -1), shared], axis=1), key_gain)
    keys = rotated_columns(keys, tables).astype(bf16)
    values = lax.dot_general(up_value, all_kv, (((0,), (1,)), ((), ())), preferred_element_type=f32).astype(bf16)
    kv = jnp.concatenate([keys, values.reshape(H, VDIM, -1)], axis=1).reshape(H * (KD + VDIM), -1)
    shift = (context_bias + math.log(TOK_DEV / CTX_DEV)) * math.log2(math.e)
    shift = jnp.broadcast_to(shift[:, None], (H, 128))
    token_rows = call(
        attend_kernel,
        3,
        jax.ShapeDtypeStruct((T, own_rows, H * VDIM), bf16),
        VM,
        [
            pltpu.VMEM((S,) + kv.shape, bf16), pltpu.VMEM((S,) + ctx.shape, bf16),
            pltpu.VMEM((H, block_tokens, 128), f32), pltpu.VMEM((H, block_tokens, 128), f32),
            pltpu.VMEM((H, block_tokens, VDIM), f32), pltpu.VMEM((block_tokens, H * VDIM), bf16),
            DMA((S,)), DMA((S,)), DMA((S,)), DMA((S,)), DMA((T,)), DMA((T,)),
        ],
        (queries, kv, ctx, shift),
    )
    token_rows = token_rows.transpose(1, 0, 2).reshape(own_rows, -1)
    projected = jnp.dot(token_rows, ow_all.reshape(-1, width), preferred_element_type=f32)
    return (latent.astype(f32) + gates * projected).astype(bf16)


def solution(mesh):
    in_specs = (
        P(("sp", "tp"), None),
        P("sp", None),
        P(),
        P(),
        P(None, "sp", "tp"),
        P(),
        P("tp", None),
        P("tp", None),
        P(),
        P(),
        P(),
        P(None, "tp"),
        P(None, "tp"),
        P(None, "tp"),
        P(),
        P(),
        P("tp"),
        P("tp", None),
    )
    out_specs = P(("sp", "tp"), None)
    return jax.shard_map(shards, mesh=mesh, in_specs=in_specs, out_specs=out_specs, check_vma=False)
```

```python
import math

import jax
import jax.numpy as jnp
from jax import lax
from jax.experimental import pallas as pl
from jax.experimental.pallas import tpu as pltpu
from jax.sharding import PartitionSpec as P

NOPE = 64
ROPE = 32
VDIM = 64
GRID_W = 64
TOK_DEV = 1024
CTX_DEV = 32


epsilon = 1e-06
theta = 10000.0


def rms_scale(tensor, gain):
    return (
        tensor
        * lax.rsqrt(jnp.mean(tensor * tensor, axis=-1, keepdims=True) + epsilon)
        * gain.astype(jnp.float32)
    )


def axial_tables(positions):
    pair_count = ROPE // 4
    frequency = jnp.power(theta, -jnp.arange(pair_count, dtype=jnp.float32) / pair_count)
    row_angle = (positions // GRID_W).astype(jnp.float32)[:, None] * frequency
    col_angle = (positions % GRID_W).astype(jnp.float32)[:, None] * frequency
    return (jnp.cos(row_angle), jnp.sin(row_angle), jnp.cos(col_angle), jnp.sin(col_angle))


def rotate_half(tensor, cosine, sine_table):
    first, second = jnp.split(tensor, 2, axis=-1)
    cosine = cosine[:, None, :]
    sine_table = sine_table[:, None, :]
    return jnp.concatenate(
        [first * cosine - second * sine_table, second * cosine + first * sine_table], axis=-1
    )


def axial_rotate(tensor, tables):
    half_width = tensor.shape[-1] // 2
    return jnp.concatenate(
        [
            rotate_half(tensor[..., :half_width], tables[0], tables[1]),
            rotate_half(tensor[..., half_width:], tables[2], tables[3]),
        ],
        axis=-1,
    )


def modulate(row_block, gain, shifts, scales):
    normal = rms_scale(row_block.astype(jnp.float32), gain)
    return (normal * (1.0 + scales) + shifts).astype(jnp.bfloat16)


def make_queries(query_latent, up_query, query_gain, tables):
    amount = query_latent.shape[0]
    projected = jnp.dot(query_latent, up_query, preferred_element_type=jnp.float32).reshape(
        amount, -1, NOPE + ROPE
    )
    normal = rms_scale(projected, query_gain)
    return jnp.concatenate(
        [normal[..., :NOPE], axial_rotate(normal[..., NOPE:], tables)], axis=-1
    ).astype(jnp.bfloat16)


def make_keys(kv_latent, rope_rows, up_key, up_value, key_gain, tables):
    amount = kv_latent.shape[0]
    unrotated = jnp.dot(kv_latent, up_key, preferred_element_type=jnp.float32).reshape(
        amount, -1, NOPE
    )
    head_count = unrotated.shape[1]
    shared = jnp.broadcast_to(rope_rows.astype(jnp.float32)[:, None, :], (amount, head_count, ROPE))
    normal = rms_scale(jnp.concatenate([unrotated, shared], axis=-1), key_gain)
    if tables is not None:
        normal = jnp.concatenate(
            [normal[..., :NOPE], axial_rotate(normal[..., NOPE:], tables)], axis=-1
        )
    values = jnp.dot(kv_latent, up_value, preferred_element_type=jnp.float32).reshape(
        amount, head_count, VDIM
    )
    return (normal.astype(jnp.bfloat16), values.astype(jnp.bfloat16))


CORES = 2


def greet(sp_peers=True):
    sp, tp = lax.axis_index("sp"), lax.axis_index("tp")
    S, T = lax.axis_size("sp"), lax.axis_size("tp")
    barrier = pltpu.get_barrier_semaphore()
    for k in range(1, S):
        pl.semaphore_signal(barrier, inc=1, device_id={"sp": lax.rem(sp + k, S)}, device_id_type=pl.DeviceIdType.MESH)
    for k in range(1, T):
        pl.semaphore_signal(barrier, inc=1, device_id={"tp": lax.rem(tp + k, T)}, device_id_type=pl.DeviceIdType.MESH)
    pl.semaphore_wait(barrier, S + T - 2)


def remote(source, target, send, recv, device):
    return pltpu.make_async_remote_copy(
        src_ref=source,
        dst_ref=target,
        send_sem=send,
        recv_sem=recv,
        device_id=device,
        device_id_type=pl.DeviceIdType.MESH,
    )


class Line:
    def __init__(self, own, slots, send, recv, z, core, Z):
        self.own, self.slots, self.send, self.recv = own, slots, send, recv
        self.z, self.core, self.Z = z, core, Z

    def hop(self, block, step, first=False):
        to = lax.max(lax.min(self.z + step, self.Z - 1), 0)
        d = 0 if step > 0 else 1
        return remote(
            self.own if first else self.slots(block),
            self.slots(block),
            self.send.at[block, d],
            self.recv.at[block],
            {"tp": to * CORES + self.core},
        )

    def start(self):
        for step in (1, -1):
            ok = (self.z + step >= 0) & (self.z + step < self.Z)

            @pl.when(ok)
            def _():
                self.hop(self.z, step, True).start()

    def each(self, body):
        for k in range(1, self.Z):
            for step in (1, -1):
                block = self.z - step * k

                @pl.when((block >= 0) & (block < self.Z))
                def _():
                    body(block, step)

    def arrive(self, block, step):
        self.hop(block, step).wait_recv()
        ok = (self.z + step >= 0) & (self.z + step < self.Z)

        @pl.when(ok)
        def _():
            self.hop(block, step).start()

    def drain(self):
        for step in (1, -1):
            ok = (self.z + step >= 0) & (self.z + step < self.Z)

            @pl.when(ok)
            def _():
                self.hop(self.z, step, True).wait_send()

        def body(block, step):
            ok = (self.z + step >= 0) & (self.z + step < self.Z)

            @pl.when(ok)
            def _():
                self.hop(block, step).wait_send()

        self.each(body)


def loop(low, high, body):
    def step(k, carry):
        body(k)
        return carry

    lax.fori_loop(low, high, step, 0)


def weights_kernel(
    act, mod_weight, dq, dkv, ow, mods, dq_all, dkv_all, ow_part,
    pm, msum, m_send, m_recv, t_send, t_recv, l_send, l_recv, s_send, s_recv, c_send, c_recv, loc,
):
    sp, tp = lax.axis_index("sp"), lax.axis_index("tp")
    S, T = lax.axis_size("sp"), lax.axis_size("tp")
    Z = T // CORES
    z, core = tp // CORES, lax.rem(tp, CORES)
    mate = {"tp": tp + 1 - 2 * core}
    for r in range(mod_weight.shape[0]):
        pm[sp, r * 8 : (r + 1) * 8, :] = jnp.dot(act[...], mod_weight[r], preferred_element_type=jnp.float32)
    greet()
    downs = ((dq, dq_all), (dkv, dkv_all))

    def part_copy(k):
        return remote(pm.at[sp], pm.at[sp], m_send.at[k], m_recv.at[k], {"sp": lax.rem(sp + k, S)})

    lines = [
        Line(a.at[sp], (lambda o: lambda b: o.at[b, core, sp])(o), l_send.at[i], l_recv.at[i], z, core, Z)
        for i, (a, o) in enumerate(downs)
    ]
    lines.append(Line(ow.at[sp], lambda b: ow_part.at[b], l_send.at[2], l_recv.at[2], z, core, Z))
    for line in lines[:2]:
        line.start()
    loop(1, S, lambda k: part_copy(k).start())
    local = []
    for i, (a, o) in enumerate(downs):
        local.append(pltpu.make_async_copy(a, o.at[z, core], loc.at[i]))
    local.append(pltpu.make_async_copy(ow.at[sp], ow_part.at[z], loc.at[2]))
    for copy in local:
        copy.start()

    def mate_copy(i, block, own=False):
        a, o = downs[i]
        return remote(
            a if own else o.at[block, core], o.at[block, core], c_send.at[i, block], c_recv.at[i, block], mate
        )

    def mate_wait(i, block):
        a, o = downs[i]
        to = o.at[block, 1 - core]
        remote(to, to, c_send.at[i, block], c_recv.at[i, block], mate).wait_recv()

    for i in range(2):
        mate_copy(i, z, True).start()

    def part_wait(k):
        to = pm.at[lax.rem(sp - k + S, S)]
        remote(to, to, m_send.at[k], m_recv.at[k], {"sp": lax.rem(sp + k, S)}).wait_recv()

    loop(1, S, part_wait)
    total = pm[0]
    for k in range(1, S):
        total = total + pm[k]
    msum[...] = total
    mods[tp] = total

    def spread(i, block, k):
        at = downs[i][1].at[block, core, sp]
        return remote(at, at, s_send.at[i, block, k], s_recv.at[i, block, k], {"sp": lax.rem(sp + k, S)})

    def gathered(i, block, k):
        at = downs[i][1].at[block, core, lax.rem(sp - k + S, S)]
        return remote(at, at, s_send.at[i, block, k], s_recv.at[i, block, k], {"sp": lax.rem(sp + k, S)})

    def body(block, step):
        for i in range(2):
            lines[i].arrive(block, step)
            loop(1, S, lambda k: spread(i, block, k).start())

    def mod_copy(k):
        return remote(msum, mods.at[tp], t_send.at[k], t_recv.at[k], {"tp": lax.rem(tp + k, T)})

    def mod_wait(k):
        to = mods.at[lax.rem(tp - k + T, T)]
        remote(msum, to, t_send.at[k], t_recv.at[k], {"tp": lax.rem(tp + k, T)}).wait_recv()

    loop(1, T, lambda k: mod_copy(k).start())
    lines[0].each(body)
    lines[2].start()
    lines[2].each(lines[2].arrive)

    def body(block, step):
        for i in range(2):
            loop(1, S, lambda k: gathered(i, block, k).wait_recv())
            mate_copy(i, block).start()

    lines[0].each(body)
    for copy in local:
        copy.wait()
    loop(1, T, mod_wait)
    for i in range(2):
        for b in range(Z):
            mate_wait(i, b)
    for i in range(2):
        mate_copy(i, z, True).wait_send()

    def body(block, step):
        for i in range(2):
            mate_copy(i, block).wait_send()
            loop(1, S, lambda k: spread(i, block, k).wait_send())

    lines[0].each(body)
    for line in lines:
        line.drain()
    loop(1, S, lambda k: part_copy(k).wait_send())
    loop(1, T, lambda k: mod_copy(k).wait_send())


def attend_kernel(
    lat_kv, lat_q, ow_part, ctx, shift, uq, ukv, pick, gain_q, gain_k, tables,
    out, ow_all,
    kv_lats, q_lats, q, kv, kv_all, ctx_all, m_scr, l_scr, acc, att,
    l_send, l_recv, c_send, c_recv, s_send, s_recv,
    k_send, k_recv, x_send, x_recv, a_send, a_recv, loc,
):
    sp, tp = lax.axis_index("sp"), lax.axis_index("tp")
    S, T = lax.axis_size("sp"), lax.axis_size("tp")
    Z = T // CORES
    z, core = tp // CORES, lax.rem(tp, CORES)
    mate = {"tp": tp + 1 - 2 * core}
    H, N, _ = q.shape
    rows = out.shape[1]
    span = rows * CORES
    KD = NOPE + ROPE
    TQ = math.gcd(N, 256)
    WIDE = KD + VDIM
    factor = KD ** (-0.5) * math.log2(math.e)
    greet()
    lats = ((lat_kv, kv_lats), (lat_q, q_lats))
    lines = [
        Line(own, (lambda o: lambda b: o.at[b, core])(every), l_send.at[i], l_recv.at[i], z, core, Z)
        for i, (own, every) in enumerate(lats)
    ]

    def mate_copy(i, block, own=False):
        to = lats[i][1].at[block, core]
        return remote(lats[i][0] if own else to, to, c_send.at[i, block], c_recv.at[i, block], mate)

    def mate_wait(i, block):
        to = lats[i][1].at[block, 1 - core]
        remote(to, to, c_send.at[i, block], c_recv.at[i, block], mate).wait_recv()

    lines[0].start()
    mate_copy(0, z, True).start()
    lines[1].start()
    mate_copy(1, z, True).start()

    def ctx_copy(k):
        return remote(ctx, ctx_all.at[sp], x_send.at[k], x_recv.at[k], {"sp": lax.rem(sp + k, S)})

    def ctx_wait(k):
        to = ctx_all.at[lax.rem(sp - k + S, S)]
        remote(ctx, to, x_send.at[k], x_recv.at[k], {"sp": lax.rem(sp + k, S)}).wait_recv()

    def kv_copy(k):
        return remote(kv, kv_all.at[sp], k_send.at[k], k_recv.at[k], {"sp": lax.rem(sp + k, S)})

    def spread(k):
        return remote(ow_part, ow_all.at[:, core, sp], s_send.at[k], s_recv.at[k], {"sp": lax.rem(sp + k, S)})

    def gathered(k):
        to = ow_all.at[:, core, lax.rem(sp - k + S, S)]
        return remote(ow_part, to, s_send.at[k], s_recv.at[k], {"sp": lax.rem(sp + k, S)})

    loop(1, S, lambda k: ctx_copy(k).start())
    loop(1, S, lambda k: spread(k).start())
    own_ow = pltpu.make_async_copy(ow_part, ow_all.at[:, core, sp], loc)
    own_ow.start()
    ctx_all[sp] = ctx[...]
    kv_lats[z, core] = lat_kv[...]
    q_lats[z, core] = lat_q[...]

    NT = (((1,), (1,)), ((), ()))

    def turned(u, gain, at):
        u = u * lax.rsqrt(jnp.mean(u * u, axis=0, keepdims=True) + epsilon) * gain[:, :1]
        m = ROPE // 4
        a, b, c, d = (u[NOPE + i * m : NOPE + (i + 1) * m, :] for i in range(4))
        rc, rs, cc, cs = (tables[i, :, at] for i in range(4))
        return jnp.concatenate(
            [u[:NOPE, :], a * rc - b * rs, b * rc + a * rs, c * cc - d * cs, d * cc + c * cs], axis=0
        )

    def passed(i):
        def body(block, step):
            lines[i].arrive(block, step)
            mate_copy(i, block).start()

        lines[i].each(body)

    passed(0)
    rank = ukv.shape[1]

    def expand_kv(b):
        mate_wait(0, b)
        at = pl.ds(pl.multiple_of(b * span, span), span)
        rows_in = kv_lats[b].reshape(span, kv_lats.shape[3])
        u = lax.dot_general(ukv[...], rows_in[:, :rank], NT, preferred_element_type=jnp.float32)
        rope = lax.dot_general(pick[...], rows_in[:, rank:], NT, preferred_element_type=jnp.float32)
        for h in range(H):
            key = turned(jnp.concatenate([u[h * NOPE : (h + 1) * NOPE, :], rope], axis=0), gain_k[...], at)
            kv[h * WIDE : h * WIDE + KD, at] = key.astype(jnp.bfloat16)
            base = H * NOPE + h * VDIM
            kv[h * WIDE + KD : (h + 1) * WIDE, at] = u[base : base + VDIM, :].astype(jnp.bfloat16)

    loop(0, Z, expand_kv)
    loop(1, S, lambda k: kv_copy(k).start())
    passed(1)

    def expand_q(b):
        mate_wait(1, b)
        at = pl.ds(pl.multiple_of(b * span, span), span)
        rows_in = q_lats[b].reshape(span, q_lats.shape[3])
        u = lax.dot_general(uq[...], rows_in, NT, preferred_element_type=jnp.float32)
        for h in range(H):
            query = turned(u[h * KD : (h + 1) * KD, :], gain_q[...], at)
            query = jnp.concatenate([query, jnp.zeros((128 - KD, span), jnp.float32)], axis=0)
            q[h, at, :] = query.T.astype(jnp.bfloat16)

    loop(0, Z, expand_q)

    def lanes(p):
        total = p[:, :128]
        for j in range(1, p.shape[1] // 128):
            total = total + p[:, j * 128 : (j + 1) * 128]
        return total

    def first(qi):
        at = pl.ds(pl.multiple_of(qi * TQ, TQ), TQ)
        for h in range(H):
            kt = kv[h * WIDE : h * WIDE + KD, :]
            vt = kv[h * WIDE + KD : (h + 1) * WIDE, :]
            s = jnp.dot(q[h, at, :][:, :KD], kt, preferred_element_type=jnp.float32) * factor
            new = jnp.max(s, axis=1, keepdims=True)
            p = jnp.exp2(s - new)
            m_scr[h, at, :] = jnp.broadcast_to(new, (TQ, 128))
            l_scr[h, at, :] = lanes(p)
            acc[h, at, :] = lax.dot_general(p.astype(jnp.bfloat16), vt, NT, preferred_element_type=jnp.float32)

    loop(0, N // TQ, first)

    def absorb(h, at, s, value, dims):
        old = m_scr[h, at, :][:, :1]
        new = jnp.maximum(old, jnp.max(s, axis=1, keepdims=True))
        scale = jnp.exp2(old - new)
        p = jnp.exp2(s - new)
        m_scr[h, at, :] = jnp.broadcast_to(new, (TQ, 128))
        l_scr[h, at, :] = l_scr[h, at, :] * scale + lanes(p)
        acc[h, at, :] = acc[h, at, :] * scale + lax.dot_general(
            p.astype(jnp.bfloat16), value, (dims, ((), ())), preferred_element_type=jnp.float32
        )

    loop(1, S, ctx_wait)

    def context_step(qi):
        at = pl.ds(pl.multiple_of(qi * TQ, TQ), TQ)
        for h in range(H):
            rows_all = ctx_all[...].reshape(-1, ctx_all.shape[2])
            kc = rows_all[:, h * 256 : h * 256 + 128][:, :KD]
            vc = rows_all[:, h * 256 + 128 : h * 256 + 256][:, :VDIM]
            s = lax.dot_general(q[h, at, :][:, :KD], kc, (((1,), (1,)), ((), ())), preferred_element_type=jnp.float32)
            s = s * factor + shift[h : h + 1, :1]
            absorb(h, at, s, vc, ((1,), (0,)))

    loop(0, N // TQ, context_step)

    def latent_step(k):
        slot = lax.rem(sp - k + S, S)
        to = kv_all.at[slot]
        remote(kv, to, k_send.at[k], k_recv.at[k], {"sp": lax.rem(sp + k, S)}).wait_recv()

        def tile(qi):
            at = pl.ds(pl.multiple_of(qi * TQ, TQ), TQ)
            for h in range(H):
                kt = kv_all[slot, h * WIDE : h * WIDE + KD, :]
                vt = kv_all[slot, h * WIDE + KD : (h + 1) * WIDE, :]
                s = jnp.dot(q[h, at, :][:, :KD], kt, preferred_element_type=jnp.float32) * factor
                absorb(h, at, s, vt, ((1,), (1,)))

        loop(0, N // TQ, tile)

    own_ow.wait()
    loop(1, S, lambda k: gathered(k).wait_recv())
    half = ow_all.at[:, core]
    whole = remote(half, half, c_send.at[0, Z], c_recv.at[0, Z], mate)
    whole.start()
    loop(1, S, latent_step)

    def finish(qi):
        at = pl.ds(pl.multiple_of(qi * TQ, TQ), TQ)
        heads = [acc[h, at, :] / jnp.sum(l_scr[h, at, :], axis=1, keepdims=True) for h in range(H)]
        att[at, :] = jnp.concatenate(heads, axis=1).astype(jnp.bfloat16)

    loop(0, N // TQ, finish)

    def give(k):
        peer = lax.rem(tp + k, T)
        return remote(
            att.at[pl.ds(pl.multiple_of(peer * rows, rows), rows)], out.at[tp], a_send.at[k], a_recv.at[k], {"tp": peer}
        )

    def take(k):
        to = out.at[lax.rem(tp - k + T, T)]
        remote(to, to, a_send.at[k], a_recv.at[k], {"tp": lax.rem(tp + k, T)}).wait_recv()

    loop(1, T, lambda k: give(k).start())
    out[tp] = att[pl.ds(pl.multiple_of(tp * rows, rows), rows), :]
    loop(1, T, take)
    loop(1, T, lambda k: give(k).wait_send())
    loop(1, S, lambda k: kv_copy(k).wait_send())
    loop(1, S, lambda k: ctx_copy(k).wait_send())
    loop(1, S, lambda k: spread(k).wait_send())
    to = ow_all.at[:, 1 - core]
    remote(to, to, c_send.at[0, Z], c_recv.at[0, Z], mate).wait_recv()
    whole.wait_send()
    for i in range(2):
        mate_copy(i, z, True).wait_send()
        lines[i].each(lambda block, step: mate_copy(i, block).wait_send())
        lines[i].drain()


DMA = pltpu.SemaphoreType.DMA
VM = pl.BlockSpec(memory_space=pltpu.VMEM)
ANY = pl.BlockSpec(memory_space=pl.ANY)


def call(kernel, ident, outs, out_specs, scratch, args):
    return pl.pallas_call(
        kernel,
        out_shape=outs,
        in_specs=[VM] * len(args),
        out_specs=out_specs,
        scratch_shapes=scratch,
        compiler_params=pltpu.CompilerParams(
            collective_id=ident, has_side_effects=True, vmem_limit_bytes=48 * 1024 * 1024
        ),
    )(*args)


def shards(
    latent, context, cond, cond_context, mod_weight, norm_gain, down_q, down_kv, rope_weight, qlat_gain, kvlat_gain,
    up_query, up_key, up_value, query_gain, key_gain, context_bias, out_weight,
):
    seq_index = lax.axis_index("sp")
    S, T = lax.axis_size("sp"), lax.axis_size("tp")
    Z = T // CORES
    bf16, f32 = jnp.bfloat16, jnp.float32
    own_rows = latent.shape[0]
    block_tokens = own_rows * T
    row_span, cols = mod_weight.shape[1:]
    width = latent.shape[1]
    activated = jax.nn.silu(jnp.stack([cond, cond_context]).astype(f32)).astype(bf16)
    own_part = lax.dynamic_slice_in_dim(activated, seq_index * row_span, row_span, 1)
    act = jnp.concatenate([own_part, jnp.zeros((6, row_span), bf16)], axis=0)
    pieces = [w.reshape(S, w.shape[0] // S, w.shape[1]) for w in (down_q, down_kv, out_weight)]
    dq, dkv, ow = pieces
    mods, dq_all, dkv_all, ow_part = call(
        weights_kernel,
        1,
        (
            jax.ShapeDtypeStruct((T, 24, cols), f32),
            jax.ShapeDtypeStruct((Z, CORES) + dq.shape, bf16),
            jax.ShapeDtypeStruct((Z, CORES) + dkv.shape, bf16),
            jax.ShapeDtypeStruct((Z,) + ow.shape[1:], bf16),
        ),
        (VM, ANY, ANY, ANY),
        [
            pltpu.VMEM((S, 24, cols), f32), pltpu.VMEM((24, cols), f32),
            DMA((S,)), DMA((S,)), DMA((T,)), DMA((T,)),
            DMA((3, Z, 2)), DMA((3, Z)), DMA((2, Z, S)), DMA((2, Z, S)), DMA((2, Z)), DMA((2, Z)), DMA((3,)),
        ],
        (act, mod_weight, dq, dkv, ow),
    )
    mods = mods.transpose(1, 0, 2).reshape(24, width)
    normed = modulate(latent, norm_gain, mods[0], mods[8])
    context_normed = modulate(context, norm_gain, mods[1], mods[9])
    gates = mods[16]
    stacked = jnp.concatenate([normed, context_normed], axis=0)
    query_down = jnp.dot(normed, dq_all.reshape(width, -1), preferred_element_type=f32)
    kv_down = jnp.dot(stacked, dkv_all.reshape(width, -1), preferred_element_type=f32)
    query_latent = rms_scale(query_down, qlat_gain).astype(bf16)
    kv_latent = rms_scale(kv_down, kvlat_gain).astype(bf16)
    rope_rows = jnp.dot(stacked, rope_weight, preferred_element_type=f32).astype(bf16)
    QR, KR = query_latent.shape[1], kv_latent.shape[1]
    lat_kv = jnp.concatenate(
        [kv_latent[:own_rows], jnp.pad(rope_rows[:own_rows], ((0, 0), (0, 128 - ROPE)))], axis=1
    )
    ctx_keys, ctx_values = make_keys(
        kv_latent[own_rows:], rope_rows[own_rows:], up_key, up_value, key_gain, None
    )
    H = ctx_keys.shape[1]
    KD = NOPE + ROPE
    ctx = jnp.concatenate(
        [jnp.pad(ctx_keys, ((0, 0), (0, 0), (0, 128 - KD))), jnp.pad(ctx_values, ((0, 0), (0, 0), (0, 128 - VDIM)))],
        axis=-1,
    ).reshape(-1, H * 256)
    positions = seq_index * block_tokens + jnp.arange(block_tokens, dtype=jnp.int32)
    tables = axial_tables(positions)
    tables = jnp.stack([table.T for table in tables])
    uq = up_query.T
    ukv = jnp.concatenate([up_key, up_value], axis=1).T
    pick = jnp.eye(ROPE, 128, dtype=bf16)
    gain_q = jnp.broadcast_to(query_gain[:, None], (KD, 128))
    gain_k = jnp.broadcast_to(key_gain[:, None], (KD, 128))
    shift = (context_bias + math.log(TOK_DEV / CTX_DEV)) * math.log2(math.e)
    shift = jnp.broadcast_to(shift[:, None], (H, 128))
    kv_rows = H * (KD + VDIM)
    token_rows, ow_all = call(
        attend_kernel,
        2,
        (
            jax.ShapeDtypeStruct((T, own_rows, H * VDIM), bf16),
            jax.ShapeDtypeStruct((Z, CORES) + ow.shape, bf16),
        ),
        (VM, ANY),
        [
            pltpu.VMEM((Z, CORES) + lat_kv.shape, bf16), pltpu.VMEM((Z, CORES) + query_latent.shape, bf16),
            pltpu.VMEM((H, block_tokens, 128), bf16), pltpu.VMEM((kv_rows, block_tokens), bf16),
            pltpu.VMEM((S, kv_rows, block_tokens), bf16), pltpu.VMEM((S,) + ctx.shape, bf16),
            pltpu.VMEM((H, block_tokens, 128), f32), pltpu.VMEM((H, block_tokens, 128), f32),
            pltpu.VMEM((H, block_tokens, VDIM), f32), pltpu.VMEM((block_tokens, H * VDIM), bf16),
            DMA((2, Z, 2)), DMA((2, Z)), DMA((2, Z + 1)), DMA((2, Z + 1)), DMA((S,)), DMA((S,)),
            DMA((S,)), DMA((S,)), DMA((S,)), DMA((S,)), DMA((T,)), DMA((T,)), DMA,
        ],
        (lat_kv, query_latent, ow_part, ctx, shift, uq, ukv, pick, gain_q, gain_k, tables),
    )
    token_rows = token_rows.transpose(1, 0, 2).reshape(own_rows, -1)
    projected = jnp.dot(token_rows, ow_all.reshape(-1, width), preferred_element_type=f32)
    return (latent.astype(f32) + gates * projected).astype(bf16)


def solution(mesh):
    in_specs = (
        P(("sp", "tp"), None),
        P("sp", None),
        P(),
        P(),
        P(None, "sp", "tp"),
        P(),
        P("tp", None),
        P("tp", None),
        P(),
        P(),
        P(),
        P(None, "tp"),
        P(None, "tp"),
        P(None, "tp"),
        P(),
        P(),
        P("tp"),
        P("tp", None),
    )
    out_specs = P(("sp", "tp"), None)
    return jax.shard_map(shards, mesh=mesh, in_specs=in_specs, out_specs=out_specs, check_vma=False)
```

```python
import math

import jax
import jax.numpy as jnp
from jax import lax
from jax.experimental import pallas as pl
from jax.experimental.pallas import tpu as pltpu
from jax.sharding import PartitionSpec as P

NOPE = 64
ROPE = 32
VDIM = 64
GRID_W = 64
TOK_DEV = 1024
CTX_DEV = 32


epsilon = 1e-06
theta = 10000.0


def rms_scale(tensor, gain):
    return (
        tensor
        * lax.rsqrt(jnp.mean(tensor * tensor, axis=-1, keepdims=True) + epsilon)
        * gain.astype(jnp.float32)
    )


def axial_tables(positions):
    pair_count = ROPE // 4
    frequency = jnp.power(theta, -jnp.arange(pair_count, dtype=jnp.float32) / pair_count)
    row_angle = (positions // GRID_W).astype(jnp.float32)[:, None] * frequency
    col_angle = (positions % GRID_W).astype(jnp.float32)[:, None] * frequency
    return (jnp.cos(row_angle), jnp.sin(row_angle), jnp.cos(col_angle), jnp.sin(col_angle))


def rotate_half(tensor, cosine, sine_table):
    first, second = jnp.split(tensor, 2, axis=-1)
    cosine = cosine[:, None, :]
    sine_table = sine_table[:, None, :]
    return jnp.concatenate(
        [first * cosine - second * sine_table, second * cosine + first * sine_table], axis=-1
    )


def axial_rotate(tensor, tables):
    half_width = tensor.shape[-1] // 2
    return jnp.concatenate(
        [
            rotate_half(tensor[..., :half_width], tables[0], tables[1]),
            rotate_half(tensor[..., half_width:], tables[2], tables[3]),
        ],
        axis=-1,
    )


def modulate(row_block, gain, shifts, scales):
    normal = rms_scale(row_block.astype(jnp.float32), gain)
    return (normal * (1.0 + scales) + shifts).astype(jnp.bfloat16)


def make_queries(query_latent, up_query, query_gain, tables):
    amount = query_latent.shape[0]
    projected = jnp.dot(query_latent, up_query, preferred_element_type=jnp.float32).reshape(
        amount, -1, NOPE + ROPE
    )
    normal = rms_scale(projected, query_gain)
    return jnp.concatenate(
        [normal[..., :NOPE], axial_rotate(normal[..., NOPE:], tables)], axis=-1
    ).astype(jnp.bfloat16)


def make_keys(kv_latent, rope_rows, up_key, up_value, key_gain, tables):
    amount = kv_latent.shape[0]
    unrotated = jnp.dot(kv_latent, up_key, preferred_element_type=jnp.float32).reshape(
        amount, -1, NOPE
    )
    head_count = unrotated.shape[1]
    shared = jnp.broadcast_to(rope_rows.astype(jnp.float32)[:, None, :], (amount, head_count, ROPE))
    normal = rms_scale(jnp.concatenate([unrotated, shared], axis=-1), key_gain)
    if tables is not None:
        normal = jnp.concatenate(
            [normal[..., :NOPE], axial_rotate(normal[..., NOPE:], tables)], axis=-1
        )
    values = jnp.dot(kv_latent, up_value, preferred_element_type=jnp.float32).reshape(
        amount, head_count, VDIM
    )
    return (normal.astype(jnp.bfloat16), values.astype(jnp.bfloat16))


CORES = 2


def greet(sp_peers=True):
    sp, tp = lax.axis_index("sp"), lax.axis_index("tp")
    S, T = lax.axis_size("sp"), lax.axis_size("tp")
    barrier = pltpu.get_barrier_semaphore()
    for k in range(1, S):
        pl.semaphore_signal(barrier, inc=1, device_id={"sp": lax.rem(sp + k, S)}, device_id_type=pl.DeviceIdType.MESH)
    for k in range(1, T):
        pl.semaphore_signal(barrier, inc=1, device_id={"tp": lax.rem(tp + k, T)}, device_id_type=pl.DeviceIdType.MESH)
    pl.semaphore_wait(barrier, S + T - 2)


def remote(source, target, send, recv, device):
    return pltpu.make_async_remote_copy(
        src_ref=source,
        dst_ref=target,
        send_sem=send,
        recv_sem=recv,
        device_id=device,
        device_id_type=pl.DeviceIdType.MESH,
    )


class Line:
    def __init__(self, own, slots, send, recv, z, core, Z):
        self.own, self.slots, self.send, self.recv = own, slots, send, recv
        self.z, self.core, self.Z = z, core, Z

    def hop(self, block, step, first=False):
        to = lax.max(lax.min(self.z + step, self.Z - 1), 0)
        d = 0 if step > 0 else 1
        return remote(
            self.own if first else self.slots(block),
            self.slots(block),
            self.send.at[block, d],
            self.recv.at[block],
            {"tp": to * CORES + self.core},
        )

    def start(self):
        for step in (1, -1):
            ok = (self.z + step >= 0) & (self.z + step < self.Z)

            @pl.when(ok)
            def _():
                self.hop(self.z, step, True).start()

    def each(self, body):
        for k in range(1, self.Z):
            for step in (1, -1):
                block = self.z - step * k

                @pl.when((block >= 0) & (block < self.Z))
                def _():
                    body(block, step)

    def arrive(self, block, step):
        self.hop(block, step).wait_recv()
        ok = (self.z + step >= 0) & (self.z + step < self.Z)

        @pl.when(ok)
        def _():
            self.hop(block, step).start()

    def drain(self):
        for step in (1, -1):
            ok = (self.z + step >= 0) & (self.z + step < self.Z)

            @pl.when(ok)
            def _():
                self.hop(self.z, step, True).wait_send()

        def body(block, step):
            ok = (self.z + step >= 0) & (self.z + step < self.Z)

            @pl.when(ok)
            def _():
                self.hop(block, step).wait_send()

        self.each(body)


def loop(low, high, body):
    def step(k, carry):
        body(k)
        return carry

    lax.fori_loop(low, high, step, 0)


def weights_kernel(
    act, mod_weight, dq, dkv, ow, mods, dq_all, dkv_all, ow_part,
    pm, msum, m_send, m_recv, t_send, t_recv, l_send, l_recv, s_send, s_recv, c_send, c_recv, loc,
):
    sp, tp = lax.axis_index("sp"), lax.axis_index("tp")
    S, T = lax.axis_size("sp"), lax.axis_size("tp")
    Z = T // CORES
    z, core = tp // CORES, lax.rem(tp, CORES)
    mate = {"tp": tp + 1 - 2 * core}
    for r in range(mod_weight.shape[0]):
        pm[sp, r * 8 : (r + 1) * 8, :] = jnp.dot(act[...], mod_weight[r], preferred_element_type=jnp.float32)
    greet()
    downs = ((dq, dq_all), (dkv, dkv_all))

    def part_copy(k):
        return remote(pm.at[sp], pm.at[sp], m_send.at[k], m_recv.at[k], {"sp": lax.rem(sp + k, S)})

    lines = [
        Line(a.at[sp], (lambda o: lambda b: o.at[b, core, sp])(o), l_send.at[i], l_recv.at[i], z, core, Z)
        for i, (a, o) in enumerate(downs)
    ]
    lines.append(Line(ow.at[sp], lambda b: ow_part.at[b], l_send.at[2], l_recv.at[2], z, core, Z))
    for line in lines[:2]:
        line.start()
    loop(1, S, lambda k: part_copy(k).start())
    local = []
    for i, (a, o) in enumerate(downs):
        local.append(pltpu.make_async_copy(a, o.at[z, core], loc.at[i]))
    local.append(pltpu.make_async_copy(ow.at[sp], ow_part.at[z], loc.at[2]))
    for copy in local:
        copy.start()

    def mate_copy(i, block, own=False):
        a, o = downs[i]
        return remote(
            a if own else o.at[block, core], o.at[block, core], c_send.at[i, block], c_recv.at[i, block], mate
        )

    def mate_wait(i, block):
        a, o = downs[i]
        to = o.at[block, 1 - core]
        remote(to, to, c_send.at[i, block], c_recv.at[i, block], mate).wait_recv()

    for i in range(2):
        mate_copy(i, z, True).start()

    def part_wait(k):
        to = pm.at[lax.rem(sp - k + S, S)]
        remote(to, to, m_send.at[k], m_recv.at[k], {"sp": lax.rem(sp + k, S)}).wait_recv()

    loop(1, S, part_wait)
    total = pm[0]
    for k in range(1, S):
        total = total + pm[k]
    msum[...] = total
    mods[tp] = total

    def spread(i, block, k):
        at = downs[i][1].at[block, core, sp]
        return remote(at, at, s_send.at[i, block, k], s_recv.at[i, block, k], {"sp": lax.rem(sp + k, S)})

    def gathered(i, block, k):
        at = downs[i][1].at[block, core, lax.rem(sp - k + S, S)]
        return remote(at, at, s_send.at[i, block, k], s_recv.at[i, block, k], {"sp": lax.rem(sp + k, S)})

    def body(block, step):
        for i in range(2):
            lines[i].arrive(block, step)
            loop(1, S, lambda k: spread(i, block, k).start())

    def mod_copy(k):
        return remote(msum, mods.at[tp], t_send.at[k], t_recv.at[k], {"tp": lax.rem(tp + k, T)})

    def mod_wait(k):
        to = mods.at[lax.rem(tp - k + T, T)]
        remote(msum, to, t_send.at[k], t_recv.at[k], {"tp": lax.rem(tp + k, T)}).wait_recv()

    loop(1, T, lambda k: mod_copy(k).start())
    lines[0].each(body)
    lines[2].start()
    lines[2].each(lines[2].arrive)

    def body(block, step):
        for i in range(2):
            loop(1, S, lambda k: gathered(i, block, k).wait_recv())
            mate_copy(i, block).start()

    lines[0].each(body)
    for copy in local:
        copy.wait()
    loop(1, T, mod_wait)
    for i in range(2):
        for b in range(Z):
            mate_wait(i, b)
    for i in range(2):
        mate_copy(i, z, True).wait_send()

    def body(block, step):
        for i in range(2):
            mate_copy(i, block).wait_send()
            loop(1, S, lambda k: spread(i, block, k).wait_send())

    lines[0].each(body)
    for line in lines:
        line.drain()
    loop(1, S, lambda k: part_copy(k).wait_send())
    loop(1, T, lambda k: mod_copy(k).wait_send())


def attend_kernel(
    lat_kv, lat_q, ow_part, ctx, shift, uq, ukv, pick, gain_q, gain_k, tables,
    out, ow_all,
    kv_lats, q_lats, q, kv, kv_all, ctx_all, m_scr, l_scr, acc, att,
    l_send, l_recv, c_send, c_recv, s_send, s_recv,
    k_send, k_recv, x_send, x_recv, a_send, a_recv, loc,
):
    sp, tp = lax.axis_index("sp"), lax.axis_index("tp")
    S, T = lax.axis_size("sp"), lax.axis_size("tp")
    Z = T // CORES
    z, core = tp // CORES, lax.rem(tp, CORES)
    mate = {"tp": tp + 1 - 2 * core}
    H, N, _ = q.shape
    rows = out.shape[1]
    span = rows * CORES
    KD = NOPE + ROPE
    TQ = math.gcd(N, 256)
    WIDE = KD + VDIM
    factor = KD ** (-0.5) * math.log2(math.e)
    greet()
    lats = ((lat_kv, kv_lats), (lat_q, q_lats))
    lines = [
        Line(own, (lambda o: lambda b: o.at[b, core])(every), l_send.at[i], l_recv.at[i], z, core, Z)
        for i, (own, every) in enumerate(lats)
    ]

    def mate_copy(i, block, own=False):
        to = lats[i][1].at[block, core]
        return remote(lats[i][0] if own else to, to, c_send.at[i, block], c_recv.at[i, block], mate)

    def mate_wait(i, block):
        to = lats[i][1].at[block, 1 - core]
        remote(to, to, c_send.at[i, block], c_recv.at[i, block], mate).wait_recv()

    lines[0].start()
    mate_copy(0, z, True).start()
    lines[1].start()
    mate_copy(1, z, True).start()

    def ctx_copy(k):
        return remote(ctx, ctx_all.at[sp], x_send.at[k], x_recv.at[k], {"sp": lax.rem(sp + k, S)})

    def ctx_wait(k):
        to = ctx_all.at[lax.rem(sp - k + S, S)]
        remote(ctx, to, x_send.at[k], x_recv.at[k], {"sp": lax.rem(sp + k, S)}).wait_recv()

    def kv_copy(k):
        return remote(kv, kv_all.at[sp], k_send.at[k], k_recv.at[k], {"sp": lax.rem(sp + k, S)})

    def spread(k):
        return remote(ow_part, ow_all.at[:, core, sp], s_send.at[k], s_recv.at[k], {"sp": lax.rem(sp + k, S)})

    def gathered(k):
        to = ow_all.at[:, core, lax.rem(sp - k + S, S)]
        return remote(ow_part, to, s_send.at[k], s_recv.at[k], {"sp": lax.rem(sp + k, S)})

    early = 1 + 2 * (S - 1) // 3
    loop(1, S, lambda k: ctx_copy(k).start())
    loop(1, early, lambda k: spread(k).start())
    own_ow = pltpu.make_async_copy(ow_part, ow_all.at[:, core, sp], loc)
    own_ow.start()
    ctx_all[sp] = ctx[...]
    kv_lats[z, core] = lat_kv[...]
    q_lats[z, core] = lat_q[...]

    NT = (((1,), (1,)), ((), ()))

    def turned(u, gain, at):
        u = u * lax.rsqrt(jnp.mean(u * u, axis=0, keepdims=True) + epsilon) * gain[:, :1]
        m = ROPE // 4
        a, b, c, d = (u[NOPE + i * m : NOPE + (i + 1) * m, :] for i in range(4))
        rc, rs, cc, cs = (tables[i, :, at] for i in range(4))
        return jnp.concatenate(
            [u[:NOPE, :], a * rc - b * rs, b * rc + a * rs, c * cc - d * cs, d * cc + c * cs], axis=0
        )

    def passed(i):
        def body(block, step):
            lines[i].arrive(block, step)
            mate_copy(i, block).start()

        lines[i].each(body)

    passed(0)
    rank = ukv.shape[1]

    def expand_kv(b):
        mate_wait(0, b)
        at = pl.ds(pl.multiple_of(b * span, span), span)
        rows_in = kv_lats[b].reshape(span, kv_lats.shape[3])
        u = lax.dot_general(ukv[...], rows_in[:, :rank], NT, preferred_element_type=jnp.float32)
        rope = lax.dot_general(pick[...], rows_in[:, rank:], NT, preferred_element_type=jnp.float32)
        for h in range(H):
            key = turned(jnp.concatenate([u[h * NOPE : (h + 1) * NOPE, :], rope], axis=0), gain_k[...], at)
            kv[h * WIDE : h * WIDE + KD, at] = key.astype(jnp.bfloat16)
            base = H * NOPE + h * VDIM
            kv[h * WIDE + KD : (h + 1) * WIDE, at] = u[base : base + VDIM, :].astype(jnp.bfloat16)

    loop(0, Z, expand_kv)
    loop(1, S, lambda k: kv_copy(k).start())
    loop(early, S, lambda k: spread(k).start())
    passed(1)

    def expand_q(b):
        mate_wait(1, b)
        at = pl.ds(pl.multiple_of(b * span, span), span)
        rows_in = q_lats[b].reshape(span, q_lats.shape[3])
        u = lax.dot_general(uq[...], rows_in, NT, preferred_element_type=jnp.float32)
        for h in range(H):
            query = turned(u[h * KD : (h + 1) * KD, :], gain_q[...], at)
            query = jnp.concatenate([query, jnp.zeros((128 - KD, span), jnp.float32)], axis=0)
            q[h, at, :] = query.T.astype(jnp.bfloat16)

    loop(0, Z, expand_q)

    def lanes(p):
        total = p[:, :128]
        for j in range(1, p.shape[1] // 128):
            total = total + p[:, j * 128 : (j + 1) * 128]
        return total

    def first(qi):
        at = pl.ds(pl.multiple_of(qi * TQ, TQ), TQ)
        for h in range(H):
            kt = kv[h * WIDE : h * WIDE + KD, :]
            vt = kv[h * WIDE + KD : (h + 1) * WIDE, :]
            s = jnp.dot(q[h, at, :][:, :KD], kt, preferred_element_type=jnp.float32) * factor
            new = jnp.max(s, axis=1, keepdims=True)
            p = jnp.exp2(s - new)
            m_scr[h, at, :] = jnp.broadcast_to(new, (TQ, 128))
            l_scr[h, at, :] = lanes(p)
            acc[h, at, :] = lax.dot_general(p.astype(jnp.bfloat16), vt, NT, preferred_element_type=jnp.float32)

    loop(0, N // TQ, first)

    def absorb(h, at, s, value, dims):
        old = m_scr[h, at, :][:, :1]
        new = jnp.maximum(old, jnp.max(s, axis=1, keepdims=True))
        scale = jnp.exp2(old - new)
        p = jnp.exp2(s - new)
        m_scr[h, at, :] = jnp.broadcast_to(new, (TQ, 128))
        l_scr[h, at, :] = l_scr[h, at, :] * scale + lanes(p)
        acc[h, at, :] = acc[h, at, :] * scale + lax.dot_general(
            p.astype(jnp.bfloat16), value, (dims, ((), ())), preferred_element_type=jnp.float32
        )

    loop(1, S, ctx_wait)

    def context_step(qi):
        at = pl.ds(pl.multiple_of(qi * TQ, TQ), TQ)
        for h in range(H):
            rows_all = ctx_all[...].reshape(-1, ctx_all.shape[2])
            kc = rows_all[:, h * 256 : h * 256 + 128][:, :KD]
            vc = rows_all[:, h * 256 + 128 : h * 256 + 256][:, :VDIM]
            s = lax.dot_general(q[h, at, :][:, :KD], kc, (((1,), (1,)), ((), ())), preferred_element_type=jnp.float32)
            s = s * factor + shift[h : h + 1, :1]
            absorb(h, at, s, vc, ((1,), (0,)))

    loop(0, N // TQ, context_step)

    def latent_step(k):
        slot = lax.rem(sp - k + S, S)
        to = kv_all.at[slot]
        remote(kv, to, k_send.at[k], k_recv.at[k], {"sp": lax.rem(sp + k, S)}).wait_recv()

        def tile(qi):
            at = pl.ds(pl.multiple_of(qi * TQ, TQ), TQ)
            for h in range(H):
                kt = kv_all[slot, h * WIDE : h * WIDE + KD, :]
                vt = kv_all[slot, h * WIDE + KD : (h + 1) * WIDE, :]
                s = jnp.dot(q[h, at, :][:, :KD], kt, preferred_element_type=jnp.float32) * factor
                absorb(h, at, s, vt, ((1,), (1,)))

        loop(0, N // TQ, tile)

    loop(1, S, latent_step)

    def finish(qi):
        at = pl.ds(pl.multiple_of(qi * TQ, TQ), TQ)
        heads = [acc[h, at, :] / jnp.sum(l_scr[h, at, :], axis=1, keepdims=True) for h in range(H)]
        att[at, :] = jnp.concatenate(heads, axis=1).astype(jnp.bfloat16)

    loop(0, N // TQ, finish)

    def give(k):
        peer = lax.rem(tp + k, T)
        return remote(
            att.at[pl.ds(pl.multiple_of(peer * rows, rows), rows)], out.at[tp], a_send.at[k], a_recv.at[k], {"tp": peer}
        )

    def take(k):
        to = out.at[lax.rem(tp - k + T, T)]
        remote(to, to, a_send.at[k], a_recv.at[k], {"tp": lax.rem(tp + k, T)}).wait_recv()

    loop(1, T, lambda k: give(k).start())
    own_ow.wait()
    loop(1, S, lambda k: gathered(k).wait_recv())
    half = ow_all.at[:, core]
    whole = remote(half, half, c_send.at[0, Z], c_recv.at[0, Z], mate)
    whole.start()
    out[tp] = att[pl.ds(pl.multiple_of(tp * rows, rows), rows), :]
    loop(1, T, take)
    loop(1, T, lambda k: give(k).wait_send())
    loop(1, S, lambda k: kv_copy(k).wait_send())
    loop(1, S, lambda k: ctx_copy(k).wait_send())
    loop(1, S, lambda k: spread(k).wait_send())
    to = ow_all.at[:, 1 - core]
    remote(to, to, c_send.at[0, Z], c_recv.at[0, Z], mate).wait_recv()
    whole.wait_send()
    for i in range(2):
        mate_copy(i, z, True).wait_send()
        lines[i].each(lambda block, step: mate_copy(i, block).wait_send())
        lines[i].drain()


DMA = pltpu.SemaphoreType.DMA
VM = pl.BlockSpec(memory_space=pltpu.VMEM)
ANY = pl.BlockSpec(memory_space=pl.ANY)


def call(kernel, ident, outs, out_specs, scratch, args, in_specs=None):
    return pl.pallas_call(
        kernel,
        out_shape=outs,
        in_specs=in_specs or [VM] * len(args),
        out_specs=out_specs,
        scratch_shapes=scratch,
        compiler_params=pltpu.CompilerParams(
            collective_id=ident, has_side_effects=True, vmem_limit_bytes=48 * 1024 * 1024
        ),
    )(*args)


def shards(
    latent, context, cond, cond_context, mod_weight, norm_gain, down_q, down_kv, rope_weight, qlat_gain, kvlat_gain,
    up_query, up_key, up_value, query_gain, key_gain, context_bias, out_weight,
):
    seq_index = lax.axis_index("sp")
    S, T = lax.axis_size("sp"), lax.axis_size("tp")
    Z = T // CORES
    bf16, f32 = jnp.bfloat16, jnp.float32
    own_rows = latent.shape[0]
    block_tokens = own_rows * T
    row_span, cols = mod_weight.shape[1:]
    width = latent.shape[1]
    activated = jax.nn.silu(jnp.stack([cond, cond_context]).astype(f32)).astype(bf16)
    own_part = lax.dynamic_slice_in_dim(activated, seq_index * row_span, row_span, 1)
    act = jnp.concatenate([own_part, jnp.zeros((6, row_span), bf16)], axis=0)
    pieces = [w.reshape(S, w.shape[0] // S, w.shape[1]) for w in (down_q, down_kv, out_weight)]
    dq, dkv, ow = pieces
    mods, dq_all, dkv_all, ow_part = call(
        weights_kernel,
        1,
        (
            jax.ShapeDtypeStruct((T, 24, cols), f32),
            jax.ShapeDtypeStruct((Z, CORES) + dq.shape, bf16),
            jax.ShapeDtypeStruct((Z, CORES) + dkv.shape, bf16),
            jax.ShapeDtypeStruct((Z,) + ow.shape[1:], bf16),
        ),
        (VM, ANY, ANY, ANY),
        [
            pltpu.VMEM((S, 24, cols), f32), pltpu.VMEM((24, cols), f32),
            DMA((S,)), DMA((S,)), DMA((T,)), DMA((T,)),
            DMA((3, Z, 2)), DMA((3, Z)), DMA((2, Z, S)), DMA((2, Z, S)), DMA((2, Z)), DMA((2, Z)), DMA((3,)),
        ],
        (act, mod_weight, dq, dkv, ow),
        [VM, VM, ANY, ANY, ANY],
    )
    mods = mods.transpose(1, 0, 2).reshape(24, width)
    normed = modulate(latent, norm_gain, mods[0], mods[8])
    context_normed = modulate(context, norm_gain, mods[1], mods[9])
    gates = mods[16]
    stacked = jnp.concatenate([normed, context_normed], axis=0)
    query_down = jnp.dot(normed, dq_all.reshape(width, -1), preferred_element_type=f32)
    kv_down = jnp.dot(stacked, dkv_all.reshape(width, -1), preferred_element_type=f32)
    query_latent = rms_scale(query_down, qlat_gain).astype(bf16)
    kv_latent = rms_scale(kv_down, kvlat_gain).astype(bf16)
    rope_rows = jnp.dot(stacked, rope_weight, preferred_element_type=f32).astype(bf16)
    QR, KR = query_latent.shape[1], kv_latent.shape[1]
    lat_kv = jnp.concatenate(
        [kv_latent[:own_rows], jnp.pad(rope_rows[:own_rows], ((0, 0), (0, 128 - ROPE)))], axis=1
    )
    ctx_keys, ctx_values = make_keys(
        kv_latent[own_rows:], rope_rows[own_rows:], up_key, up_value, key_gain, None
    )
    H = ctx_keys.shape[1]
    KD = NOPE + ROPE
    ctx = jnp.concatenate(
        [jnp.pad(ctx_keys, ((0, 0), (0, 0), (0, 128 - KD))), jnp.pad(ctx_values, ((0, 0), (0, 0), (0, 128 - VDIM)))],
        axis=-1,
    ).reshape(-1, H * 256)
    positions = seq_index * block_tokens + jnp.arange(block_tokens, dtype=jnp.int32)
    tables = axial_tables(positions)
    tables = jnp.stack([table.T for table in tables])
    uq = up_query.T
    ukv = jnp.concatenate([up_key, up_value], axis=1).T
    pick = jnp.eye(ROPE, 128, dtype=bf16)
    gain_q = jnp.broadcast_to(query_gain[:, None], (KD, 128))
    gain_k = jnp.broadcast_to(key_gain[:, None], (KD, 128))
    shift = (context_bias + math.log(TOK_DEV / CTX_DEV)) * math.log2(math.e)
    shift = jnp.broadcast_to(shift[:, None], (H, 128))
    kv_rows = H * (KD + VDIM)
    token_rows, ow_all = call(
        attend_kernel,
        2,
        (
            jax.ShapeDtypeStruct((T, own_rows, H * VDIM), bf16),
            jax.ShapeDtypeStruct((Z, CORES) + ow.shape, bf16),
        ),
        (VM, ANY),
        [
            pltpu.VMEM((Z, CORES) + lat_kv.shape, bf16), pltpu.VMEM((Z, CORES) + query_latent.shape, bf16),
            pltpu.VMEM((H, block_tokens, 128), bf16), pltpu.VMEM((kv_rows, block_tokens), bf16),
            pltpu.VMEM((S, kv_rows, block_tokens), bf16), pltpu.VMEM((S,) + ctx.shape, bf16),
            pltpu.VMEM((H, block_tokens, 128), f32), pltpu.VMEM((H, block_tokens, 128), f32),
            pltpu.VMEM((H, block_tokens, VDIM), f32), pltpu.VMEM((block_tokens, H * VDIM), bf16),
            DMA((2, Z, 2)), DMA((2, Z)), DMA((2, Z + 1)), DMA((2, Z + 1)), DMA((S,)), DMA((S,)),
            DMA((S,)), DMA((S,)), DMA((S,)), DMA((S,)), DMA((T,)), DMA((T,)), DMA,
        ],
        (lat_kv, query_latent, ow_part, ctx, shift, uq, ukv, pick, gain_q, gain_k, tables),
    )
    token_rows = token_rows.transpose(1, 0, 2).reshape(own_rows, -1)
    projected = jnp.dot(token_rows, ow_all.reshape(-1, width), preferred_element_type=f32)
    return (latent.astype(f32) + gates * projected).astype(bf16)


def solution(mesh):
    in_specs = (
        P(("sp", "tp"), None),
        P("sp", None),
        P(),
        P(),
        P(None, "sp", "tp"),
        P(),
        P("tp", None),
        P("tp", None),
        P(),
        P(),
        P(),
        P(None, "tp"),
        P(None, "tp"),
        P(None, "tp"),
        P(),
        P(),
        P("tp"),
        P("tp", None),
    )
    out_specs = P(("sp", "tp"), None)
    return jax.shard_map(shards, mesh=mesh, in_specs=in_specs, out_specs=out_specs, check_vma=False)
```
